768 devices in a mesh: sp: 24 (over z, core), tp: 32 (over y, x).
Axes of the slice: x: 4, y: 8, z: 12, core: 2. Of those that a mesh axis runs over, the one named last changes fastest.
Arguments:
- context_activations: bfloat16 [2, 6144, 4096], P(None, 'sp', 'tp'), may hold values from -6 to 6
- first_generated_activation: bfloat16 [2, 4096], replicated, may hold values from -6 to 6
- address_projection: bfloat16 [4096, 4096], P(None, 'tp'), may hold values from -0.09375 to 0.09375
- payload_projection: bfloat16 [4096, 4096], P(None, 'tp'), may hold values from -0.09375 to 0.09375
- lookup_projection: bfloat16 [4096, 4096], P(None, 'tp'), may hold values from -0.09375 to 0.09375
- exit_gating_projection: bfloat16 [4096, 4096], P(None, 'tp'), may hold values from -0.09375 to 0.09375
- writing_intensity_projection: bfloat16 [4096, 32], replicated, may hold values from -0.09375 to 0.09375
- fading_projection: bfloat16 [4096, 32], replicated, may hold values from -0.09375 to 0.09375
- channel_fading_speed: float32 [32], replicated, may hold values from 0 to 1, as said below
- extra_fading_log: float32 [2, 6144, 32], P(None, 'sp', 'tp'), may hold values from -1 to 0, as said below
- readout_normalizer_gain: float32 [128], replicated, may hold values from 0.1 to 1.9
- exit_projection: bfloat16 [4096, 4096], P('tp'), may hold values from -0.09375 to 0.09375
Outputs:
- state_cache: bfloat16 [2, 24, 32, 128, 128], P(None, 'sp', 'tp')
- step_out: bfloat16 [2, 4096], P(None, 'tp')
The draws below stay inside these ranges and needn't reach their ends.
Inputs may be any that keep to these rules, and one draw needn't show every extreme that they name: `channel_fading_speed`: positive rates, one a head. `extra_fading_log`: zero at all but a few positions of each prompt and head, negative there.
All inputs are finite; a program needn't handle non-finite values.
Results may differ from the reference program's by a relative error of at most 0.012.
Values may be sent and summed in bfloat16 or wider, within the bound.
A program may use at most 64 MiB of HBM per device.

```python
import math
import jax
import jax.numpy as jnp
from jax import lax

D = 4096
HEAD = 128
BLOCK = 64
PROMPT_TOTAL = 2
SEG = 256
HEAD_TOTAL = 32
PROMPT_LENGTH = 6144


def draw_channel_fading_speed(key, part):
    pick_key, level_key = jax.random.split(jax.random.fold_in(key, 11))
    level = jax.random.uniform(level_key, (HEAD_TOTAL,), jnp.float32)
    slow_low = math.log(0.15 / (0.7 * PROMPT_LENGTH))
    slow_high = math.log(1.2 / (0.7 * PROMPT_LENGTH))
    slow_rate = jnp.exp(slow_low + level * (slow_high - slow_low))
    fast_low = math.log(1.0 / (0.7 * 50.0))
    fast_high = math.log(1.0 / (0.7 * 25.0))
    fast_rate = jnp.exp(fast_low + level * (fast_high - fast_low))
    which = jax.random.uniform(pick_key, (HEAD_TOTAL,), jnp.float32) < 0.5
    return jnp.where(which, fast_rate, slow_rate)


def draw_extra_fading_log(key, part):
    start_random_key, length_random_key = jax.random.split(jax.random.fold_in(key, 23))
    segment_start = jax.random.randint(start_random_key, (PROMPT_TOTAL, 1, HEAD_TOTAL, 2), 0, PROMPT_LENGTH)
    segment_length = jax.random.uniform(length_random_key, (PROMPT_TOTAL, 1, HEAD_TOTAL, 2), jnp.float32, -0.69, -0.22)
    split_places = jnp.arange(PROMPT_LENGTH)[None, :, None, None]
    return jnp.sum(jnp.where(split_places == segment_start, segment_length, 0.0), axis=-1)


def block_scale(own_key, dims, shards, smallest, top_value):
    loudness, own = 1.0, jax.random.fold_in(own_key, 6)
    for position, parts in shards:
        draws = jnp.exp(jax.random.uniform(jax.random.fold_in(own, position), (parts,), jnp.float32, smallest / len(shards), top_value / len(shards)))
        loudness = loudness * jnp.repeat(draws, dims[position] // parts).reshape([-1 if axis == position else 1 for axis in range(len(dims))])
    return loudness


def noise(stream_key, dims, deviation, limit, shards=(), kind=jnp.bfloat16):
    level = block_scale(stream_key, dims, shards, -0.22, 0.18) if shards else 1.0
    entries = jax.random.normal(stream_key, dims, jnp.float32) * deviation * level
    return jnp.minimum(jnp.maximum(entries, -limit), limit).astype(kind)


def setup_inputs(seed: int = 0) -> dict:
    keys = jax.random.split(jax.random.key(seed), 13)
    return {
        "context_activations": noise(keys[0], (PROMPT_TOTAL, PROMPT_LENGTH, D), 1.0, 6.0, ((1, 24), (2, 32))),
        "first_generated_activation": noise(keys[1], (PROMPT_TOTAL, D), 1.0, 6.0),
        "address_projection": noise(keys[2], (D, HEAD_TOTAL * HEAD), D ** -0.5, 0.09375, ((1, 32),)),
        "payload_projection": noise(keys[3], (D, HEAD_TOTAL * HEAD), D ** -0.5, 0.09375, ((1, 32),)),
        "lookup_projection": noise(keys[4], (D, HEAD_TOTAL * HEAD), D ** -0.5, 0.09375, ((1, 32),)),
        "exit_gating_projection": noise(keys[5], (D, HEAD_TOTAL * HEAD), D ** -0.5, 0.09375, ((1, 32),)),
        "writing_intensity_projection": noise(keys[6], (D, HEAD_TOTAL), D ** -0.5, 0.09375),
        "fading_projection": noise(keys[7], (D, HEAD_TOTAL), D ** -0.5, 0.09375),
        "channel_fading_speed": draw_channel_fading_speed(jax.random.fold_in(keys[12], 71), 0),
        "extra_fading_log": draw_extra_fading_log(jax.random.fold_in(keys[12], 71), 0),
        "readout_normalizer_gain": jnp.clip(1.0 + 0.18 * jax.random.normal(keys[10], (HEAD,), jnp.float32), 0.1, 1.9),
        "exit_projection": noise(keys[11], (HEAD_TOTAL * HEAD, D), (HEAD_TOTAL * HEAD) ** -0.5, 0.09375, ((0, 32),)),
    }


norm_eps = 1e-06
highest = lax.Precision.HIGHEST

def unit_rows(values_in):
    return values_in * lax.rsqrt(lax.optimization_barrier(jnp.sum(values_in * values_in, axis=-1, keepdims=True)) + norm_eps)

def boundary_states(keys_in, values_in, beta_gate, fading_exponent):
    blocks = keys_in.shape[0] // BLOCK
    key_blocks = keys_in.reshape(blocks, BLOCK, -1)
    value_blocks = values_in.reshape(blocks, BLOCK, -1)
    beta_blocks = beta_gate.reshape(blocks, BLOCK)
    cumul = jnp.cumsum(fading_exponent.reshape(blocks, BLOCK), axis=-1)
    causal = jnp.tril(jnp.ones((BLOCK, BLOCK), bool))
    strict = jnp.tril(jnp.ones((BLOCK, BLOCK), bool), -1)
    gaps_log = cumul[:, :, None] - cumul[:, None, :]
    within = jnp.where(causal, jnp.exp(jnp.where(causal, gaps_log, 0.0)), 0.0)
    keys_beta = key_blocks * beta_blocks[..., None]
    strict_part = jnp.where(strict, jnp.einsum('nid,njd->nij', keys_beta, key_blocks, precision=highest) * within, 0.0)
    targets = jnp.concatenate([value_blocks * beta_blocks[..., None], keys_beta * jnp.exp(cumul)[..., None]], axis=-1)
    system = jnp.eye(BLOCK, dtype=jnp.float32) + strict_part
    solved = lax.linalg.triangular_solve(system, targets, left_side=True, lower=True)
    width_v = value_blocks.shape[-1]
    pseudo_values = solved[..., :width_v]
    decayed_keys = solved[..., width_v:]
    trailing = key_blocks * jnp.exp(cumul[:, -1:] - cumul)[..., None]
    block_decay = jnp.exp(cumul[:, -1])

    def advance(memory, inputs):
        pseudo, decayed, trail_keys, shrink = inputs
        fresh_values = pseudo - jnp.dot(decayed, memory, precision=highest)
        memory = memory * shrink + jnp.dot(trail_keys.T, fresh_values, precision=highest)
        return (memory, memory)
    start_state = jnp.zeros((key_blocks.shape[-1], width_v), jnp.float32)
    _, every = lax.scan(advance, start_state, (pseudo_values, decayed_keys, trailing, block_decay))
    per_run = SEG // BLOCK
    return every[per_run - 1::per_run]

def one_sequence(inputs):
    keys_one, values_one, beta_one, decay_one = inputs
    return jax.vmap(boundary_states, in_axes=(1, 1, 1, 1), out_axes=1)(keys_one.astype(jnp.float32), values_one.astype(jnp.float32), beta_one, decay_one)

def reference(context_activations, first_generated_activation, address_projection, payload_projection, lookup_projection, exit_gating_projection, writing_intensity_projection, fading_projection, channel_fading_speed, extra_fading_log, readout_normalizer_gain, exit_projection):
    seq_count, length, width = context_activations.shape
    head_count = channel_fading_speed.shape[0]
    head_size = readout_normalizer_gain.shape[0]
    tokens = context_activations.reshape(seq_count * length, width)
    shaped = (seq_count, length, head_count, head_size)
    prompt_keys = unit_rows(jax.nn.silu(jnp.dot(tokens.astype(jnp.float32), address_projection.astype(jnp.float32), preferred_element_type=jnp.float32)).reshape(shaped)).astype(jnp.bfloat16)
    prompt_values = jax.nn.silu(jnp.dot(tokens.astype(jnp.float32), payload_projection.astype(jnp.float32), preferred_element_type=jnp.float32)).reshape(shaped).astype(jnp.bfloat16)
    beta_logit = jnp.dot(tokens.astype(jnp.float32), writing_intensity_projection.astype(jnp.float32), preferred_element_type=jnp.float32).astype(jnp.bfloat16).reshape(seq_count, length, head_count)
    fading_logit_entry = jnp.dot(tokens.astype(jnp.float32), fading_projection.astype(jnp.float32), preferred_element_type=jnp.float32).astype(jnp.bfloat16).reshape(seq_count, length, head_count)
    beta_gate = jax.nn.sigmoid(beta_logit.astype(jnp.float32))
    fading_exponent = extra_fading_log - channel_fading_speed * jax.nn.softplus(fading_logit_entry.astype(jnp.float32))
    runs = lax.map(one_sequence, (prompt_keys, prompt_values, beta_gate, fading_exponent))
    state_cache = runs.astype(jnp.bfloat16)
    states = runs[:, -1]
    heads_shape = (seq_count, head_count, head_size)
    new_keys = unit_rows(jax.nn.silu(jnp.dot(first_generated_activation.astype(jnp.float32), address_projection.astype(jnp.float32), preferred_element_type=jnp.float32)).reshape(heads_shape))
    new_values = jax.nn.silu(jnp.dot(first_generated_activation.astype(jnp.float32), payload_projection.astype(jnp.float32), preferred_element_type=jnp.float32)).reshape(heads_shape)
    new_queries = unit_rows(jax.nn.silu(jnp.dot(first_generated_activation.astype(jnp.float32), lookup_projection.astype(jnp.float32), preferred_element_type=jnp.float32)).reshape(heads_shape))
    out_gate = jax.nn.silu(jnp.dot(first_generated_activation.astype(jnp.float32), exit_gating_projection.astype(jnp.float32), preferred_element_type=jnp.float32)).reshape(heads_shape)
    new_beta = jax.nn.sigmoid(jnp.dot(first_generated_activation.astype(jnp.float32), writing_intensity_projection.astype(jnp.float32), preferred_element_type=jnp.float32))
    new_decay = jnp.exp(-channel_fading_speed * jax.nn.softplus(jnp.dot(first_generated_activation.astype(jnp.float32), fading_projection.astype(jnp.float32), preferred_element_type=jnp.float32)))
    recalled = jnp.einsum('shk,shkv->shv', new_keys, states, precision=highest)
    updated = new_decay[..., None, None] * (states - new_beta[..., None, None] * new_keys[..., None] * recalled[:, :, None, :])
    updated = updated + new_beta[..., None, None] * new_keys[..., None] * new_values[:, :, None, :]
    read = jnp.einsum('shk,shkv->shv', new_queries, updated, precision=highest)
    normed = read * lax.rsqrt(lax.optimization_barrier(jnp.mean(read * read, axis=-1, keepdims=True)) + norm_eps) * readout_normalizer_gain * out_gate
    normed = normed.astype(jnp.bfloat16).reshape(seq_count, head_count * head_size)
    step_out = jnp.dot(normed.astype(jnp.float32), exit_projection.astype(jnp.float32), preferred_element_type=jnp.float32).astype(jnp.bfloat16)
    return (state_cache, step_out)
```

```python
import jax
import jax.numpy as jnp
from jax import lax
from jax.experimental import pallas as pl
from jax.experimental.pallas import tpu as pltpu
from jax.sharding import Mesh
from jax.sharding import PartitionSpec as P

NZ, NC, NY, NX = 12, 2, 8, 4
NT = NY * NX
HEAD = 128
RUN = 256
ROWS = 2 * RUN
WIDTH = NT * 128
KEEP = NX * 128
PIECES = 4
UP, DOWN = 6, 5
MESH = pl.DeviceIdType.MESH
f32, bf16 = jnp.float32, jnp.bfloat16
norm_eps = 1e-06

A = (0, 192)
A_HALF = ((0, 96), (96, 96))
B = (192, 320)
B_HALF = ((192, 160), (352, 160))


def dot(a, b):
    return jnp.dot(a, b, preferred_element_type=f32)


def dot_nt(a, b):
    return lax.dot_general(a, b, (((1,), (1,)), ((), ())), preferred_element_type=f32)


def split(a):
    high = a.astype(bf16)
    return high, (a - high.astype(f32)).astype(bf16)


def wide_left(a):
    high, low = split(a)
    return jnp.concatenate([high, low], axis=1)


def dot_ff(a, b):
    high, low = split(b)
    both = jnp.concatenate([high, low], axis=1)
    out = dot(wide_left(a), jnp.concatenate([both, both], axis=0))
    return out[:, :128] + out[:, 128:]


def dot_fb(a, b):
    return dot(wide_left(a), jnp.concatenate([b, b], axis=0))


def dot_bf(a, b):
    high, low = split(b)
    return dot(jnp.concatenate([a, a], axis=1), jnp.concatenate([high, low], axis=0))


def silu(v):
    return v / (1.0 + jnp.exp(-v))


def sigmoid(v):
    return 1.0 / (1.0 + jnp.exp(-v))


def softplus(v):
    return jnp.maximum(v, 0.0) + jnp.log1p(jnp.exp(-jnp.abs(v)))


def unit(v):
    return v * lax.rsqrt(jnp.sum(v * v, axis=-1, keepdims=True) + norm_eps)


def iota(shape, dim):
    return lax.broadcasted_iota(jnp.int32, shape, dim)


def inverses(systems):
    row, col = iota((128, 128), 0), iota((128, 128), 1)
    eye = (row == col).astype(f32)

    def lower_blocks(bits):
        r, c = row >> bits, col >> bits
        return (r == c + 1) & ((r & 1) == 1)

    found = [eye - jnp.where(lower_blocks(0), a, 0.0) for a in systems]
    for bits in range(1, 7):
        chosen = lower_blocks(bits)
        right = [dot_ff(jnp.where(chosen, a, 0.0), t) for a, t in zip(systems, found)]
        found = [t - dot_ff(t, r) for t, r in zip(found, right)]
    return found


def run_maps(keys, values, beta_logits, decay_logits, extra_rows, speed):
    row, col = iota((RUN, RUN), 0), iota((RUN, RUN), 1)
    causal = row >= col
    systems, trails, betas, grown, lasts = [], [], [], [], []
    for p in range(2):
        beta_col = sigmoid(beta_logits[p])
        pace_col = softplus(decay_logits[p])
        pace_row = jnp.sum(jnp.where(row == col, pace_col, 0.0), axis=0, keepdims=True)
        fade_row = extra_rows[p] - speed * pace_row
        cum_col = jnp.sum(jnp.where(causal, fade_row, 0.0), axis=1, keepdims=True)
        cum_row = jnp.sum(jnp.where(row == col, cum_col, 0.0), axis=0, keepdims=True)
        beta_row = jnp.sum(jnp.where(row == col, beta_col, 0.0), axis=0, keepdims=True)
        last = cum_row[:, RUN - 1 :]
        within = jnp.where(causal, jnp.exp(jnp.where(causal, cum_col - cum_row, 0.0)), 0.0)
        gram = dot_nt(keys[p], keys[p])
        systems.append(jnp.where(row > col, gram * within * beta_col, 0.0))
        trails.append(keys[p].astype(f32).T * jnp.exp(last - cum_row))
        betas.append(beta_row)
        grown.append(jnp.exp(cum_row))
        lasts.append(jnp.exp(last))
    solved = inverses([systems[0][:128, :128], systems[0][128:, 128:],
                       systems[1][:128, :128], systems[1][128:, 128:]])
    maps = []
    diagonal = iota((128, 128), 0) == iota((128, 128), 1)
    for p in range(2):
        second = dot_ff(trails[p][:, 128:], solved[2 * p + 1])
        first = trails[p][:, :128] - dot_ff(second, systems[p][128:, :128])
        first = dot_ff(first, solved[2 * p])
        writes = jnp.concatenate([first, second], axis=1) * betas[p]
        offset = dot_fb(writes, values[p])
        moves = jnp.where(diagonal, lasts[p], 0.0) - dot_fb(writes * grown[p], keys[p])
        maps.append(jnp.concatenate([moves, offset], axis=1))
    return maps


def kernel(
    x_hbm, fg_hbm, wk_hbm, wv_hbm, wq_hbm, wz_hbm, wb_hbm, wd_hbm, speeds, extra_hbm, gain_hbm, wo_hbm,
    cache_ref, step_ref,
    chunks, wkv, wqz, wlogit, wl, wo, fg, extra, gain,
    acc, acc_l, facc, own_map, other_map, blocks, state_out, state_in, parts_out, parts_in, row_out, row_in,
    load_sem, gather_send, ax_sem, ay_sem, by_sem, bx_sem,
    swap_send, swap_recv, ring_send, up_sem, down_sem, part_send, part_recv,
):
    z, c = lax.axis_index("z"), lax.axis_index("c")
    y, x = lax.axis_index("y"), lax.axis_index("x")
    mine = y * NX + x

    def ring(at, step, size):
        return lax.rem(at + (step % size), size)

    def slot(yy, xx):
        return yy * NX + xx

    def load(src, dst, sem):
        copy = pltpu.make_async_copy(src, dst, load_sem.at[sem])
        copy.start()
        return copy

    own_load = load(x_hbm, chunks.at[mine], 0)
    logit_loads = [
        load(wb_hbm, wlogit.at[pl.ds(0, 32)], 1),
        load(wd_hbm, wlogit.at[pl.ds(32, 32)], 2),
    ]
    early_loads = [
        load(fg_hbm, fg, 3),
        load(wk_hbm, wkv.at[:, pl.ds(0, 128)], 4),
        load(wv_hbm, wkv.at[:, pl.ds(128, 128)], 5),
        load(wq_hbm, wqz.at[:, pl.ds(0, 128)], 6),
        load(wz_hbm, wqz.at[:, pl.ds(128, 128)], 7),
    ]
    late_loads = [load(extra_hbm, extra, 8), load(gain_hbm, gain, 9), load(wo_hbm, wo, 10)]

    barrier = pltpu.get_barrier_semaphore()

    def greet(d, carry):
        other = lax.rem(mine + d, NT)
        pl.semaphore_signal(
            barrier, inc=1, device_id={"y": other // NX, "x": lax.rem(other, NX)}, device_id_type=MESH
        )
        return carry

    lax.fori_loop(1, NT, greet, 0)
    pl.semaphore_signal(barrier, inc=1, device_id={"z": ring(z, 1, NZ)}, device_id_type=MESH)
    pl.semaphore_signal(barrier, inc=1, device_id={"z": ring(z, -1, NZ)}, device_id_type=MESH)
    pl.semaphore_signal(barrier, inc=1, device_id={"c": 1 - c}, device_id_type=MESH)

    for copy in logit_loads:
        copy.wait()
    pick_row, pick_col = iota((16, 64), 0), iota((16, 64), 1)
    pick = ((pick_row == 0) & (pick_col == mine)) | ((pick_row == 1) & (pick_col == mine + 32))
    wl[...] = dot(jnp.where(pick, 1.0, 0.0).astype(bf16), wlogit[...]).astype(bf16)
    own_load.wait()
    pl.semaphore_wait(barrier, NT - 1 + 3)

    y_to = ({"y": ring(y, 1, NY)}, {"y": ring(y, -1, NY)})
    x_to = ({"x": ring(x, 1, NX)}, {"x": ring(x, -1, NX)})
    sign = (-1, 1)

    def chunk_copy(yy, xx, rows, sem, to):
        view = chunks.at[slot(yy, xx), pl.ds(rows[0], rows[1])]
        return pltpu.make_async_remote_copy(
            src_ref=view, dst_ref=view, send_sem=gather_send, recv_sem=sem, device_id=to, device_id_type=MESH
        )

    def ax(k, h, start):
        xx = ring(x, sign[k] * (h - 1 if start else h), NX)
        copy = chunk_copy(y, xx, A if h < 2 else A_HALF[k], ax_sem.at[k, h - 1], x_to[k])
        copy.start() if start else copy.wait_recv()

    def ay(k, h, j, start):
        yy = ring(y, sign[k] * (h - 1 if start else h), NY)
        copy = chunk_copy(yy, ring(x, j, NX), A if h < 4 else A_HALF[k], ay_sem.at[k, h - 1, j], y_to[k])
        copy.start() if start else copy.wait_recv()

    def by(k, h, start):
        yy = ring(y, sign[k] * (h - 1 if start else h), NY)
        copy = chunk_copy(yy, x, B if h < 4 else B_HALF[k], by_sem.at[k, h - 1], y_to[k])
        copy.start() if start else copy.wait_recv()

    def bx(k, h, j, start):
        xx = ring(x, sign[k] * (h - 1 if start else h), NX)
        copy = chunk_copy(ring(y, j, NY), xx, B if h < 2 else B_HALF[k], bx_sem.at[k, h - 1, j % NY], x_to[k])
        copy.start() if start else copy.wait_recv()

    both = (0, 1)

    def project(steps):
        def one(yy):
            row = pl.multiple_of(yy * KEEP, KEEP)
            left = jnp.concatenate([chunks[yy * NX + i] for i in range(NX)], axis=1)
            acc[...] += dot(left, wkv[pl.ds(row, KEEP), :])
            acc_l[...] += dot_nt(left, wl[:, pl.ds(row, KEEP)])

        for step in steps:
            one(ring(y, step, NY))

    def bx_first(j):
        for k in both:
            bx(k, 1, j, False)
            bx(k, 2, j, True)

    def bx_last(j):
        for k in both:
            bx(k, 2, j, False)

    def ay_pass(h, j):
        for k in both:
            ay(k, h, j, False)
            if h < 4:
                ay(k, h + 1, j, True)

    def by_pass(h):
        for k in both:
            by(k, h, False)
            if h < 4:
                by(k, h + 1, True)
        for j in (-h, h) if h < 4 else (4,):
            for k in both:
                bx(k, 1, j, True)

    for k in both:
        by(k, 1, True)
        ax(k, 1, True)
    for k in both:
        bx(k, 1, 0, True)
        ay(k, 1, 0, True)

    for copy in early_loads:
        copy.wait()
    facc[...] = jnp.zeros_like(facc)
    acc[...] = jnp.zeros_like(acc)
    acc_l[...] = jnp.zeros_like(acc_l)

    def first_step(i, carry):
        at = pl.multiple_of(i * KEEP, KEEP)
        left = fg[:, pl.ds(at, KEEP)]
        facc[:, 0:256] += dot(left, wkv[pl.ds(at, KEEP), :])
        facc[:, 256:512] += dot(left, wqz[pl.ds(at, KEEP), :])
        facc[:, 512:528] += dot_nt(left, wl[:, pl.ds(at, KEEP)])
        return carry

    lax.fori_loop(0, WIDTH // KEEP, first_step, 0)

    for k in both:
        ax(k, 1, False)
        ax(k, 2, True)
    for k in both:
        ay(k, 1, 1, True)
        ay(k, 1, 3, True)
    by_pass(1)
    bx_first(0)
    ay_pass(1, 0)
    for k in both:
        ax(k, 2, False)
    for k in both:
        ay(k, 1, 2, True)
    by_pass(2)
    ay_pass(1, 1)
    ay_pass(1, 3)
    bx_first(-1)
    bx_first(1)
    bx_last(0)
    ay_pass(1, 2)
    by_pass(3)
    ay_pass(2, 0)
    ay_pass(2, 1)
    project([0])
    ay_pass(2, 3)
    bx_first(-2)
    bx_first(2)
    bx_last(-1)
    bx_last(1)
    ay_pass(2, 2)
    by_pass(4)
    ay_pass(3, 0)
    project([-1])
    ay_pass(3, 1)
    ay_pass(3, 3)
    bx_first(-3)
    bx_first(3)
    project([1])
    ay_pass(3, 2)
    bx_last(-2)
    bx_last(2)
    bx_first(4)
    project([-2, 2])
    bx_last(-3)
    bx_last(3)
    project([-3, 3])
    for j in range(NX):
        ay_pass(4, j)
    bx_last(4)
    project([4])

    for copy in late_loads:
        copy.wait()
    speed = speeds[mine]
    keys = unit(silu(acc[:, 0:128])).astype(bf16)
    values = silu(acc[:, 128:256]).astype(bf16)
    logits = acc_l[...].astype(bf16).astype(f32)
    maps = run_maps(
        [keys[:RUN], keys[RUN:]],
        [values[:RUN], values[RUN:]],
        [logits[:RUN, 0:1], logits[RUN:, 0:1]],
        [logits[:RUN, 1:2], logits[RUN:, 1:2]],
        [extra[0], extra[1]],
        speed,
    )

    own_map[0] = maps[0]
    own_map[1] = maps[1]

    def swap(src, dst, i):
        return pltpu.make_async_remote_copy(
            src_ref=src, dst_ref=dst, send_sem=swap_send.at[i], recv_sem=swap_recv.at[i],
            device_id={"c": 1 - c}, device_id_type=MESH,
        )

    map_swap = swap(own_map.at[1 - c], other_map, 0)
    map_swap.start()

    my_row = iota((2, 1), 0) == c

    def chosen(lo, hi):
        return jnp.sum(jnp.where(my_row, facc[:, lo:hi], 0.0), axis=0, keepdims=True)

    new_key = unit(silu(chosen(0, 128)))
    new_value = silu(chosen(128, 256))
    new_query = unit(silu(chosen(256, 384)))
    out_gate = silu(chosen(384, 512))
    new_beta = sigmoid(chosen(512, 513))
    new_decay = jnp.exp(-speed * softplus(chosen(513, 514)))
    meeting = jnp.sum(new_key * new_query, axis=-1, keepdims=True)
    carried_query = new_decay * (new_query - new_beta * new_key * meeting)
    own_write = new_beta * new_value * meeting

    map_swap.wait()
    here = jnp.where(c == 0, maps[0], maps[1])
    there = other_map[...]
    early = jnp.where(c == 0, here, there)
    late = jnp.where(c == 0, there, here)
    zeros = jnp.zeros((128, 128), f32)

    def with_offset(product, offset):
        return jnp.concatenate([product[:, :128], product[:, 128:] + offset], axis=1)

    pair = jnp.concatenate(
        [dot_ff(late[:, :128], early[:, :128]), dot_ff(late[:, :128], early[:, 128:]) + late[:, 128:]], axis=1
    )
    blocks[z] = pair.astype(bf16)

    z_to = ({"z": ring(z, 1, NZ)}, {"z": ring(z, -1, NZ)})
    piece_rows = 128 // PIECES
    z_sem = (up_sem, down_sem)

    def hop(k, h, q, start):
        zz = ring(z, sign[k] * (h - 1 if start else h), NZ)
        view = blocks.at[zz, pl.ds(q * piece_rows, piece_rows)]
        copy = pltpu.make_async_remote_copy(
            src_ref=view, dst_ref=view, send_sem=ring_send, recv_sem=z_sem[k].at[h - 1, q],
            device_id=z_to[k], device_id_type=MESH,
        )
        copy.start() if start else copy.wait_recv()

    limit = (UP, DOWN)
    for q in range(PIECES):
        for k in both:
            hop(k, 1, q, True)

    eye = (iota((128, 128), 0) == iota((128, 128), 1)).astype(f32)
    before = jnp.concatenate([eye, zeros], axis=1)
    reader = jnp.concatenate(
        [jnp.where(iota((8, 128), 0) == 0, carried_query, 0.0), jnp.zeros((8, 128), f32)], axis=1
    )
    after = before
    start_state = jnp.concatenate([zeros, zeros], axis=1)
    for h in range(1, UP + 1):
        for q in range(PIECES):
            for k in both:
                if h <= limit[k]:
                    hop(k, h, q, False)
                    if h < limit[k]:
                        hop(k, h + 1, q, True)
        block = blocks[ring(z, -h, NZ)]
        stacked = jnp.concatenate([before, reader], axis=0)
        grown = with_offset(dot_fb(stacked[:, :128], block), stacked[:, 128:])
        earlier = z >= h
        before = jnp.where(earlier, grown[:128], before)
        reader = jnp.where(earlier, reader, grown[128:])
        if h <= DOWN:
            block = blocks[ring(z, h, NZ)]
            later = z + h < NZ
            taken = jnp.where(later, after, start_state)
            grown = dot_bf(block[:, :128], taken)
            grown = with_offset(grown, block[:, 128:].astype(f32))
            after = jnp.where(later, grown, after)
            start_state = jnp.where(later, start_state, grown)

    entering = dot_ff(before[:, :128], start_state[:, 128:]) + before[:, 128:]
    leaving = dot_ff(jnp.concatenate([early[:, :128], pair[:, :128]], axis=0), entering)
    state_first = leaving[:128] + early[:, 128:]
    state_second = leaving[128:] + pair[:, 128:]

    state_out[...] = jnp.where(c == 0, state_second, state_first).astype(bf16)
    state_swap = swap(state_out, state_in, 1)
    state_swap.start()

    final_map = jnp.concatenate(
        [dot_ff(reader[:, :128], after[:, :128]), dot_ff(reader[:, :128], after[:, 128:])], axis=1
    )
    read = dot_ff(final_map[:, :128], state_second) + final_map[:, 128:] + reader[:, 128:]
    read = read[0:1] + own_write
    normed = read * lax.rsqrt(jnp.mean(read * read, axis=-1, keepdims=True) + norm_eps) * gain[...] * out_gate
    normed = jnp.broadcast_to(normed, (8, 128)).astype(bf16)
    partial = dot(normed, wo[...])
    for t in range(NT):
        parts_out[t] = partial[0:1, t * 128 : (t + 1) * 128]

    def part(d):
        other = lax.rem(mine + d, NT)
        return pltpu.make_async_remote_copy(
            src_ref=parts_out.at[other], dst_ref=parts_in.at[d - 1], send_sem=part_send, recv_sem=part_recv,
            device_id={"y": other // NX, "x": lax.rem(other, NX)}, device_id_type=MESH,
        )

    def send_part(d, carry):
        part(d).start()
        return carry

    lax.fori_loop(1, NT, send_part, 0)
    state_swap.wait()
    kept = jnp.where(c == 0, state_first, state_second).astype(bf16)
    came = state_in[...]
    cache_ref[0] = jnp.where(c == 0, kept, came)
    cache_ref[1] = jnp.where(c == 0, came, kept)
    total = parts_out[mine]
    pltpu.make_async_copy(parts_in, parts_in, part_recv).wait()
    total = total + jnp.sum(parts_in[...], axis=0)
    row_out[...] = total
    row_swap = swap(row_out, row_in, 2)
    row_swap.start()
    row_swap.wait()
    step_ref[...] = jnp.where(my_row, total, row_in[...]).astype(bf16)

    sent = chunks.at[pl.ds(0, NT - 1)]
    pltpu.make_async_copy(sent, sent, gather_send).wait()
    sent = blocks.at[pl.ds(0, UP + DOWN)]
    pltpu.make_async_copy(sent, sent, ring_send).wait()
    pltpu.make_async_copy(parts_in, parts_in, part_send).wait()


def body(
    context_activations,
    first_generated_activation,
    address_projection,
    payload_projection,
    lookup_projection,
    exit_gating_projection,
    writing_intensity_projection,
    fading_projection,
    channel_fading_speed,
    extra_fading_log,
    readout_normalizer_gain,
    exit_projection,
):
    hbm = pl.BlockSpec(memory_space=pl.ANY)
    vmem = pl.BlockSpec(memory_space=pltpu.VMEM)
    dma = pltpu.SemaphoreType.DMA
    cache, step = pl.pallas_call(
        kernel,
        out_shape=(jax.ShapeDtypeStruct((2, HEAD, HEAD), bf16), jax.ShapeDtypeStruct((2, 128), bf16)),
        in_specs=[hbm] * 8 + [pl.BlockSpec(memory_space=pltpu.SMEM)] + [hbm] * 3,
        out_specs=(vmem, vmem),
        scratch_shapes=[
            pltpu.VMEM((NT, ROWS, 128), bf16),
            pltpu.VMEM((WIDTH, 256), bf16),
            pltpu.VMEM((WIDTH, 256), bf16),
            pltpu.VMEM((64, WIDTH), bf16),
            pltpu.VMEM((16, WIDTH), bf16),
            pltpu.VMEM((HEAD, WIDTH), bf16),
            pltpu.VMEM((2, WIDTH), bf16),
            pltpu.VMEM((2, 1, RUN), f32),
            pltpu.VMEM((1, HEAD), f32),
            pltpu.VMEM((ROWS, 256), f32),
            pltpu.VMEM((ROWS, 16), f32),
            pltpu.VMEM((2, 528), f32),
            pltpu.VMEM((2, 128, 256), f32),
            pltpu.VMEM((128, 256), f32),
            pltpu.VMEM((NZ, 128, 256), bf16),
            pltpu.VMEM((128, 128), bf16),
            pltpu.VMEM((128, 128), bf16),
            pltpu.VMEM((NT, 1, 128), f32),
            pltpu.VMEM((NT - 1, 1, 128), f32),
            pltpu.VMEM((1, 128), f32),
            pltpu.VMEM((1, 128), f32),
            dma((11,)),
            dma,
            dma((2, 2)),
            dma((2, 4, NX)),
            dma((2, 4)),
            dma((2, 2, NY)),
            dma((3,)),
            dma((3,)),
            dma,
            dma((UP, PIECES)),
            dma((DOWN, PIECES)),
            dma,
            dma,
        ],
        compiler_params=pltpu.CompilerParams(
            collective_id=0, has_side_effects=True, vmem_limit_bytes=40 * 1024 * 1024
        ),
    )(
        context_activations.reshape(ROWS, 128),
        first_generated_activation,
        address_projection,
        payload_projection,
        lookup_projection,
        exit_gating_projection,
        writing_intensity_projection.T,
        fading_projection.T,
        channel_fading_speed,
        jnp.transpose(extra_fading_log, (0, 2, 1)),
        readout_normalizer_gain.reshape(1, HEAD),
        exit_projection,
    )
    return cache.reshape(2, 1, 1, HEAD, HEAD), step


def solution(mesh):
    torus = Mesh(mesh.devices.reshape(NZ, NC, NY, NX), ("z", "c", "y", "x"))
    SP, TP = ("z", "c"), ("y", "x")
    in_specs = (
        P(None, SP, TP),
        P(),
        P(None, TP),
        P(None, TP),
        P(None, TP),
        P(None, TP),
        P(),
        P(),
        P(),
        P(None, SP, TP),
        P(),
        P(TP, None),
    )
    out_specs = (P(None, SP, TP, None, None), P(None, TP))
    return jax.shard_map(body, mesh=torus, in_specs=in_specs, out_specs=out_specs, check_vma=False)
```

```python
import jax
import jax.numpy as jnp
from jax import lax
from jax.experimental import pallas as pl
from jax.experimental.pallas import tpu as pltpu
from jax.sharding import Mesh
from jax.sharding import PartitionSpec as P

NZ, NC, NY, NX = 12, 2, 8, 4
NT = NY * NX
HEAD = 128
RUN = 256
ROWS = 2 * RUN
WIDTH = NT * 128
KEEP = NX * 128
PIECES = 4
UP, DOWN = 6, 5
MESH = pl.DeviceIdType.MESH
f32, bf16 = jnp.float32, jnp.bfloat16
norm_eps = 1e-06

A = (0, 208)
A_HALF = ((0, 112), (112, 96))
B = (208, 304)
B_HALF = ((208, 144), (352, 160))


def dot(a, b):
    return jnp.dot(a, b, preferred_element_type=f32)


def dot_nt(a, b):
    return lax.dot_general(a, b, (((1,), (1,)), ((), ())), preferred_element_type=f32)


def split(a):
    high = a.astype(bf16)
    return high, (a - high.astype(f32)).astype(bf16)


def wide_left(a):
    high, low = split(a)
    return jnp.concatenate([high, low], axis=1)


def dot_ff(a, b):
    high, low = split(b)
    both = jnp.concatenate([high, low], axis=1)
    out = dot(wide_left(a), jnp.concatenate([both, both], axis=0))
    return out[:, :128] + out[:, 128:]


def dot_fb(a, b):
    return dot(wide_left(a), jnp.concatenate([b, b], axis=0))


def dot_bf(a, b):
    high, low = split(b)
    return dot(jnp.concatenate([a, a], axis=1), jnp.concatenate([high, low], axis=0))


def silu(v):
    return v / (1.0 + jnp.exp(-v))


def sigmoid(v):
    return 1.0 / (1.0 + jnp.exp(-v))


def softplus(v):
    return jnp.maximum(v, 0.0) + jnp.log1p(jnp.exp(-jnp.abs(v)))


def unit(v):
    return v * lax.rsqrt(jnp.sum(v * v, axis=-1, keepdims=True) + norm_eps)


def iota(shape, dim):
    return lax.broadcasted_iota(jnp.int32, shape, dim)


def inverses(systems):
    row, col = iota((128, 128), 0), iota((128, 128), 1)
    eye = (row == col).astype(f32)

    def lower_blocks(bits):
        r, c = row >> bits, col >> bits
        return (r == c + 1) & ((r & 1) == 1)

    found = [eye - jnp.where(lower_blocks(0), a, 0.0) for a in systems]
    for bits in range(1, 7):
        chosen = lower_blocks(bits)
        right = [dot_ff(jnp.where(chosen, a, 0.0), t) for a, t in zip(systems, found)]
        found = [t - dot_ff(t, r) for t, r in zip(found, right)]
    return found


def run_maps(keys, values, beta_logits, decay_logits, extra_rows, speed):
    row, col = iota((RUN, RUN), 0), iota((RUN, RUN), 1)
    causal = row >= col
    systems, trails, betas, grown, lasts = [], [], [], [], []
    for p in range(2):
        beta_col = sigmoid(beta_logits[p])
        pace_col = softplus(decay_logits[p])
        pace_row = jnp.sum(jnp.where(row == col, pace_col, 0.0), axis=0, keepdims=True)
        fade_row = extra_rows[p] - speed * pace_row
        cum_col = jnp.sum(jnp.where(causal, fade_row, 0.0), axis=1, keepdims=True)
        cum_row = jnp.sum(jnp.where(row == col, cum_col, 0.0), axis=0, keepdims=True)
        beta_row = jnp.sum(jnp.where(row == col, beta_col, 0.0), axis=0, keepdims=True)
        last = cum_row[:, RUN - 1 :]
        within = jnp.where(causal, jnp.exp(jnp.where(causal, cum_col - cum_row, 0.0)), 0.0)
        gram = dot_nt(keys[p], keys[p])
        systems.append(jnp.where(row > col, gram * within * beta_col, 0.0))
        trails.append(keys[p].astype(f32).T * jnp.exp(last - cum_row))
        betas.append(beta_row)
        grown.append(jnp.exp(cum_row))
        lasts.append(jnp.exp(last))
    solved = inverses([systems[0][:128, :128], systems[0][128:, 128:],
                       systems[1][:128, :128], systems[1][128:, 128:]])
    maps = []
    diagonal = iota((128, 128), 0) == iota((128, 128), 1)
    for p in range(2):
        second = dot_ff(trails[p][:, 128:], solved[2 * p + 1])
        first = trails[p][:, :128] - dot_ff(second, systems[p][128:, :128])
        first = dot_ff(first, solved[2 * p])
        writes = jnp.concatenate([first, second], axis=1) * betas[p]
        offset = dot_fb(writes, values[p])
        moves = jnp.where(diagonal, lasts[p], 0.0) - dot_fb(writes * grown[p], keys[p])
        maps.append(jnp.concatenate([moves, offset], axis=1))
    return maps


def kernel(
    x_hbm, fg_hbm, wk_hbm, wv_hbm, wq_hbm, wz_hbm, wb_hbm, wd_hbm, speed_hbm, extra_hbm, gain_hbm, wo_hbm,
    cache_ref, step_ref,
    chunks, wkv, wqz, wlogit, wl, wo, fg, extra, gain, speeds,
    acc, acc_l, facc, own_map, other_map, blocks, state_out, state_in, parts_out, parts_in, row_out, row_in,
    load_sem, gather_send, ax_sem, ay_sem, by_sem, bx_sem,
    swap_send, swap_recv, ring_send, up_sem, down_sem, part_send, part_recv,
):
    z, c = lax.axis_index("z"), lax.axis_index("c")
    y, x = lax.axis_index("y"), lax.axis_index("x")
    mine = y * NX + x

    def ring(at, step, size):
        return lax.rem(at + (step % size), size)

    def slot(yy, xx):
        return yy * NX + xx

    def load(src, dst, sem):
        copy = pltpu.make_async_copy(src, dst, load_sem.at[sem])
        copy.start()
        return copy

    own_load = load(x_hbm, chunks.at[mine], 0)
    logit_loads = [
        load(wb_hbm, wlogit.at[pl.ds(0, 32)], 1),
        load(wd_hbm, wlogit.at[pl.ds(32, 32)], 2),
    ]
    early_loads = [
        load(fg_hbm, fg, 3),
        load(wk_hbm, wkv.at[:, pl.ds(0, 128)], 4),
        load(wv_hbm, wkv.at[:, pl.ds(128, 128)], 5),
        load(wq_hbm, wqz.at[:, pl.ds(0, 128)], 6),
        load(wz_hbm, wqz.at[:, pl.ds(128, 128)], 7),
    ]
    late_loads = [
        load(extra_hbm, extra, 8), load(gain_hbm, gain, 9), load(wo_hbm, wo, 10), load(speed_hbm, speeds, 11)
    ]

    barrier = pltpu.get_barrier_semaphore()
    for axis, at, size in (("x", x, NX), ("y", y, NY), ("z", z, NZ)):
        for step in (1, -1):
            pl.semaphore_signal(barrier, inc=1, device_id={axis: ring(at, step, size)}, device_id_type=MESH)
    pl.semaphore_signal(barrier, inc=1, device_id={"c": 1 - c}, device_id_type=MESH)
    own_load.wait()
    pl.semaphore_wait(barrier, 7)

    y_to = ({"y": ring(y, 1, NY)}, {"y": ring(y, -1, NY)})
    x_to = ({"x": ring(x, 1, NX)}, {"x": ring(x, -1, NX)})
    sign = (-1, 1)

    def chunk_copy(yy, xx, rows, sem, to):
        view = chunks.at[slot(yy, xx), pl.ds(rows[0], rows[1])]
        return pltpu.make_async_remote_copy(
            src_ref=view, dst_ref=view, send_sem=gather_send, recv_sem=sem, device_id=to, device_id_type=MESH
        )

    def ax(k, h, start):
        xx = ring(x, sign[k] * (h - 1 if start else h), NX)
        copy = chunk_copy(y, xx, A if h < 2 else A_HALF[k], ax_sem.at[k, h - 1], x_to[k])
        copy.start() if start else copy.wait_recv()

    def ay(k, h, j, start):
        yy = ring(y, sign[k] * (h - 1 if start else h), NY)
        copy = chunk_copy(yy, ring(x, j, NX), A if h < 4 else A_HALF[k], ay_sem.at[k, h - 1, j], y_to[k])
        copy.start() if start else copy.wait_recv()

    def by(k, h, start):
        yy = ring(y, sign[k] * (h - 1 if start else h), NY)
        copy = chunk_copy(yy, x, B if h < 4 else B_HALF[k], by_sem.at[k, h - 1], y_to[k])
        copy.start() if start else copy.wait_recv()

    def bx(k, h, j, start):
        xx = ring(x, sign[k] * (h - 1 if start else h), NX)
        copy = chunk_copy(ring(y, j, NY), xx, B if h < 2 else B_HALF[k], bx_sem.at[k, h - 1, j % NY], x_to[k])
        copy.start() if start else copy.wait_recv()

    both = (0, 1)

    def project(steps):
        def one(yy):
            row = pl.multiple_of(yy * KEEP, KEEP)
            left = jnp.concatenate([chunks[yy * NX + i] for i in range(NX)], axis=1)
            acc[...] += dot(left, wkv[pl.ds(row, KEEP), :])
            acc_l[...] += dot_nt(left, wl[:, pl.ds(row, KEEP)])

        for step in steps:
            one(ring(y, step, NY))

    def bx_first(j):
        for k in both:
            bx(k, 1, j, False)
            bx(k, 2, j, True)

    def bx_last(j):
        for k in both:
            bx(k, 2, j, False)

    def ay_pass(h, j):
        for k in both:
            ay(k, h, j, False)
            if h < 4:
                ay(k, h + 1, j, True)

    def by_pass(h):
        for k in both:
            by(k, h, False)
            if h < 4:
                by(k, h + 1, True)
        for j in (-h, h) if h < 4 else (4,):
            for k in both:
                bx(k, 1, j, True)

    for k in both:
        by(k, 1, True)
        ax(k, 1, True)
    for k in both:
        bx(k, 1, 0, True)
        ay(k, 1, 0, True)

    for copy in logit_loads:
        copy.wait()
    pick_row, pick_col = iota((16, 64), 0), iota((16, 64), 1)
    pick = ((pick_row == 0) & (pick_col == mine)) | ((pick_row == 1) & (pick_col == mine + 32))
    wl[...] = dot(jnp.where(pick, 1.0, 0.0).astype(bf16), wlogit[...]).astype(bf16)
    facc[...] = jnp.zeros_like(facc)
    acc[...] = jnp.zeros_like(acc)
    acc_l[...] = jnp.zeros_like(acc_l)

    def first_step(i, carry):
        at = pl.multiple_of(i * KEEP, KEEP)
        left = fg[:, pl.ds(at, KEEP)]
        facc[:, 0:256] += dot(left, wkv[pl.ds(at, KEEP), :])
        facc[:, 256:512] += dot(left, wqz[pl.ds(at, KEEP), :])
        facc[:, 512:528] += dot_nt(left, wl[:, pl.ds(at, KEEP)])
        return carry

    for k in both:
        ax(k, 1, False)
        ax(k, 2, True)
    for k in both:
        ay(k, 1, 1, True)
        ay(k, 1, 3, True)
    by_pass(1)
    bx_first(0)
    ay_pass(1, 0)
    for k in both:
        ax(k, 2, False)
    for k in both:
        ay(k, 1, 2, True)
    by_pass(2)
    ay_pass(1, 1)
    ay_pass(1, 3)
    bx_first(-1)
    bx_first(1)
    bx_last(0)
    ay_pass(1, 2)
    by_pass(3)
    ay_pass(2, 0)
    ay_pass(2, 1)
    for copy in early_loads:
        copy.wait()
    project([0])
    ay_pass(2, 3)
    bx_first(-2)
    bx_first(2)
    bx_last(-1)
    bx_last(1)
    ay_pass(2, 2)
    by_pass(4)
    lax.fori_loop(0, 4, first_step, 0)
    ay_pass(3, 0)
    project([-1])
    ay_pass(3, 1)
    ay_pass(3, 3)
    bx_first(-3)
    bx_first(3)
    project([1])
    ay_pass(3, 2)
    bx_last(-2)
    bx_last(2)
    bx_first(4)
    lax.fori_loop(4, 8, first_step, 0)
    project([-2, 2])
    bx_last(-3)
    bx_last(3)
    project([-3, 3])
    for j in range(NX):
        ay_pass(4, j)
    bx_last(4)
    project([4])

    for copy in late_loads:
        copy.wait()
    speed = jnp.sum(jnp.where(iota((1, NT), 1) == mine, speeds[...], 0.0), axis=1, keepdims=True)
    keys = unit(silu(acc[:, 0:128])).astype(bf16)
    values = silu(acc[:, 128:256]).astype(bf16)
    logits = acc_l[...].astype(bf16).astype(f32)
    maps = run_maps(
        [keys[:RUN], keys[RUN:]],
        [values[:RUN], values[RUN:]],
        [logits[:RUN, 0:1], logits[RUN:, 0:1]],
        [logits[:RUN, 1:2], logits[RUN:, 1:2]],
        [extra[0], extra[1]],
        speed,
    )

    other_core = {"c": 1 - c}

    def swap(src, dst, i):
        return pltpu.make_async_remote_copy(
            src_ref=src, dst_ref=dst, send_sem=swap_send.at[i], recv_sem=swap_recv.at[i],
            device_id=other_core, device_id_type=MESH,
        )

    both_prompts = (0, 1)
    map_swap = swap(own_map, other_map, 0)
    state_swap = swap(state_out, state_in, 1)
    row_swap = swap(row_out, row_in, 2)

    @pl.when(c == 0)
    def _():
        own_map[0] = maps[0]
        own_map[1] = maps[1]
        map_swap.start()
        state_swap.wait_recv()
        cache_ref[...] = state_in[...]
        row_swap.wait_recv()
        step_ref[...] = row_in[...].astype(bf16)
        map_swap.wait_send()

    @pl.when(c == 1)
    def _():
        first = facc[...]
        new_key = unit(silu(first[:, 0:128]))
        new_value = silu(first[:, 128:256])
        new_query = unit(silu(first[:, 256:384]))
        out_gate = silu(first[:, 384:512])
        new_beta = sigmoid(first[:, 512:513])
        new_decay = jnp.exp(-speed * softplus(first[:, 513:514]))
        meeting = jnp.sum(new_key * new_query, axis=-1, keepdims=True)
        carried_query = new_decay * (new_query - new_beta * new_key * meeting)
        own_write = new_beta * new_value * meeting

        zeros = jnp.zeros((128, 128), f32)
        eye = (iota((128, 128), 0) == iota((128, 128), 1)).astype(f32)

        def with_offset(product, offset):
            return jnp.concatenate([product[:, :128], product[:, 128:] + offset], axis=1)

        z_to = ({"z": ring(z, 1, NZ)}, {"z": ring(z, -1, NZ)})
        z_sem = (up_sem, down_sem)
        per_prompt = PIECES // 2
        piece_rows = 128 // per_prompt

        def hop(k, h, q, start):
            zz = ring(z, sign[k] * (h - 1 if start else h), NZ)
            view = blocks.at[zz, q // per_prompt, pl.ds(q % per_prompt * piece_rows, piece_rows)]
            copy = pltpu.make_async_remote_copy(
                src_ref=view, dst_ref=view, send_sem=ring_send, recv_sem=z_sem[k].at[h - 1, q],
                device_id=z_to[k], device_id_type=MESH,
            )
            copy.start() if start else copy.wait_recv()

        map_swap.wait_recv()
        pair = []
        for p in both_prompts:
            early, late = other_map[p], maps[p]
            product = [dot_ff(late[:, :128], early[:, i * 128 : (i + 1) * 128]) for i in range(2)]
            pair.append(jnp.concatenate([product[0], product[1] + late[:, 128:]], axis=1))
            blocks[z, p] = pair[p].astype(bf16)
        for q in range(PIECES):
            for k in both:
                hop(k, 1, q, True)

        limit = (UP, DOWN)
        before = [jnp.concatenate([eye, zeros], axis=1)] * 2
        after = [jnp.concatenate([eye, zeros], axis=1)] * 2
        start_state = [jnp.concatenate([zeros, zeros], axis=1)] * 2
        reader = [
            jnp.concatenate(
                [jnp.where(iota((8, 128), 0) == 0, carried_query[p : p + 1], 0.0), jnp.zeros((8, 128), f32)], axis=1
            )
            for p in both_prompts
        ]
        for h in range(1, UP + 1):
            for p in both_prompts:
                for q in range(p * per_prompt, (p + 1) * per_prompt):
                    for k in both:
                        if h <= limit[k]:
                            hop(k, h, q, False)
                            if h < limit[k]:
                                hop(k, h + 1, q, True)
                block = blocks[ring(z, -h, NZ), p]
                stacked = jnp.concatenate([before[p], reader[p]], axis=0)
                grown = with_offset(dot_fb(stacked[:, :128], block), stacked[:, 128:])
                earlier = z >= h
                before[p] = jnp.where(earlier, grown[:128], before[p])
                reader[p] = jnp.where(earlier, reader[p], grown[128:])
                if h <= DOWN:
                    block = blocks[ring(z, h, NZ), p]
                    later = z + h < NZ
                    taken = jnp.where(later, after[p], start_state[p])
                    grown = dot_bf(block[:, :128], taken)
                    grown = with_offset(grown, block[:, 128:].astype(f32))
                    after[p] = jnp.where(later, grown, after[p])
                    start_state[p] = jnp.where(later, start_state[p], grown)

        seconds, reads = [], []
        for p in both_prompts:
            entering = dot_ff(before[p][:, :128], start_state[p][:, 128:]) + before[p][:, 128:]
            second = dot_ff(pair[p][:, :128], entering) + pair[p][:, 128:]
            early = other_map[p]
            state_out[p] = (dot_ff(early[:, :128], entering) + early[:, 128:]).astype(bf16)
            tail = [dot_ff(reader[p][:, :128], after[p][:, i * 128 : (i + 1) * 128]) for i in range(2)]
            read = dot_ff(tail[0], second) + tail[1] + reader[p][:, 128:]
            seconds.append(second)
            reads.append(read[0:1])
        state_swap.start()
        read = jnp.concatenate(reads, axis=0) + own_write
        normed = read * lax.rsqrt(jnp.mean(read * read, axis=-1, keepdims=True) + norm_eps) * gain[...] * out_gate
        partial = dot(normed.astype(bf16), wo[...])
        for t in range(NT):
            parts_out[t] = partial[:, t * 128 : (t + 1) * 128]

        def send_part(d, carry):
            other = lax.rem(mine + d, NT)
            pltpu.make_async_remote_copy(
                src_ref=parts_out.at[other], dst_ref=parts_in.at[d - 1], send_sem=part_send, recv_sem=part_recv,
                device_id={"y": other // NX, "x": lax.rem(other, NX)}, device_id_type=MESH,
            ).start()
            return carry

        lax.fori_loop(1, NT, send_part, 0)
        for p in both_prompts:
            cache_ref[p] = seconds[p].astype(bf16)
        total = parts_out[mine]
        pltpu.make_async_copy(parts_in, parts_in, part_recv).wait()
        total = total + jnp.sum(parts_in[...], axis=0)
        row_out[...] = total
        row_swap.start()
        step_ref[...] = total.astype(bf16)
        state_swap.wait_send()
        row_swap.wait_send()
        sent = blocks.at[pl.ds(0, UP + DOWN)]
        pltpu.make_async_copy(sent, sent, ring_send).wait()
        pltpu.make_async_copy(parts_in, parts_in, part_send).wait()

    sent = chunks.at[pl.ds(0, NT - 1)]
    pltpu.make_async_copy(sent, sent, gather_send).wait()


def body(
    context_activations,
    first_generated_activation,
    address_projection,
    payload_projection,
    lookup_projection,
    exit_gating_projection,
    writing_intensity_projection,
    fading_projection,
    channel_fading_speed,
    extra_fading_log,
    readout_normalizer_gain,
    exit_projection,
):
    hbm = pl.BlockSpec(memory_space=pltpu.HBM)
    vmem = pl.BlockSpec(memory_space=pltpu.VMEM)
    dma = pltpu.SemaphoreType.DMA
    cache, step = pl.pallas_call(
        kernel,
        out_shape=(jax.ShapeDtypeStruct((2, HEAD, HEAD), bf16), jax.ShapeDtypeStruct((2, 128), bf16)),
        in_specs=[hbm] * 12,
        out_specs=(vmem, vmem),
        scratch_shapes=[
            pltpu.VMEM((NT, ROWS, 128), bf16),
            pltpu.VMEM((WIDTH, 256), bf16),
            pltpu.VMEM((WIDTH, 256), bf16),
            pltpu.VMEM((64, WIDTH), bf16),
            pltpu.VMEM((16, WIDTH), bf16),
            pltpu.VMEM((HEAD, WIDTH), bf16),
            pltpu.VMEM((2, WIDTH), bf16),
            pltpu.VMEM((2, 1, RUN), f32),
            pltpu.VMEM((1, HEAD), f32),
            pltpu.VMEM((1, NT), f32),
            pltpu.VMEM((ROWS, 256), f32),
            pltpu.VMEM((ROWS, 16), f32),
            pltpu.VMEM((2, 528), f32),
            pltpu.VMEM((2, 128, 256), f32),
            pltpu.VMEM((2, 128, 256), f32),
            pltpu.VMEM((NZ, 2, 128, 256), bf16),
            pltpu.VMEM((2, 128, 128), bf16),
            pltpu.VMEM((2, 128, 128), bf16),
            pltpu.VMEM((NT, 2, 128), f32),
            pltpu.VMEM((NT - 1, 2, 128), f32),
            pltpu.VMEM((2, 128), f32),
            pltpu.VMEM((2, 128), f32),
            dma((12,)),
            dma,
            dma((2, 2)),
            dma((2, 4, NX)),
            dma((2, 4)),
            dma((2, 2, NY)),
            dma((3,)),
            dma((3,)),
            dma,
            dma((UP, PIECES)),
            dma((DOWN, PIECES)),
            dma,
            dma,
        ],
        compiler_params=pltpu.CompilerParams(
            collective_id=0, has_side_effects=True, vmem_limit_bytes=67_043_328
        ),
    )(
        context_activations.reshape(ROWS, 128),
        first_generated_activation,
        address_projection,
        payload_projection,
        lookup_projection,
        exit_gating_projection,
        writing_intensity_projection.T,
        fading_projection.T,
        channel_fading_speed.reshape(1, NT),
        jnp.transpose(extra_fading_log, (0, 2, 1)),
        readout_normalizer_gain.reshape(1, HEAD),
        exit_projection,
    )
    return cache.reshape(2, 1, 1, HEAD, HEAD), step


def solution(mesh):
    torus = Mesh(mesh.devices.reshape(NZ, NC, NY, NX), ("z", "c", "y", "x"))
    SP, TP = ("z", "c"), ("y", "x")
    in_specs = (
        P(None, SP, TP),
        P(),
        P(None, TP),
        P(None, TP),
        P(None, TP),
        P(None, TP),
        P(),
        P(),
        P(),
        P(None, SP, TP),
        P(),
        P(TP, None),
    )
    out_specs = (P(None, SP, TP, None, None), P(None, TP))
    return jax.shard_map(body, mesh=torus, in_specs=in_specs, out_specs=out_specs, check_vma=False)
```

```python
import jax
import jax.numpy as jnp
from jax import lax
from jax.experimental import pallas as pl
from jax.experimental.pallas import tpu as pltpu
from jax.sharding import Mesh
from jax.sharding import PartitionSpec as P

NZ, NC, NY, NX = 12, 2, 8, 4
NT = NY * NX
HEAD = 128
RUN = 256
ROWS = 2 * RUN
WIDTH = NT * 128
KEEP = NX * 128
PIECES = 8
UP, DOWN = 6, 5
MESH = pl.DeviceIdType.MESH
f32, bf16 = jnp.float32, jnp.bfloat16
norm_eps = 1e-06

A = (0, 208)
A_HALF = ((0, 112), (112, 96))
B = (208, 304)
B_HALF = ((208, 144), (352, 160))


def dot(a, b):
    return jnp.dot(a, b, preferred_element_type=f32)


def dot_nt(a, b):
    return lax.dot_general(a, b, (((1,), (1,)), ((), ())), preferred_element_type=f32)


def split(a):
    high = a.astype(bf16)
    return high, (a - high.astype(f32)).astype(bf16)


def wide_left(a):
    high, low = split(a)
    return jnp.concatenate([high, low], axis=1)


def dot_ff(a, b):
    high, low = split(b)
    both = jnp.concatenate([high, low], axis=1)
    out = dot(wide_left(a), jnp.concatenate([both, both], axis=0))
    return out[:, :128] + out[:, 128:]


def dot_fb(a, b):
    return dot(wide_left(a), jnp.concatenate([b, b], axis=0))


def dot_bf(a, b):
    high, low = split(b)
    return dot(jnp.concatenate([a, a], axis=1), jnp.concatenate([high, low], axis=0))


def silu(v):
    return v / (1.0 + jnp.exp(-v))


def sigmoid(v):
    return 1.0 / (1.0 + jnp.exp(-v))


def softplus(v):
    return jnp.maximum(v, 0.0) + jnp.log1p(jnp.exp(-jnp.abs(v)))


def unit(v):
    return v * lax.rsqrt(jnp.sum(v * v, axis=-1, keepdims=True) + norm_eps)


def iota(shape, dim):
    return lax.broadcasted_iota(jnp.int32, shape, dim)


def inverses(systems):
    row, col = iota((128, 128), 0), iota((128, 128), 1)
    eye = (row == col).astype(f32)

    def lower_blocks(bits):
        r, c = row >> bits, col >> bits
        return (r == c + 1) & ((r & 1) == 1)

    found = [eye - jnp.where(lower_blocks(0), a, 0.0) for a in systems]
    for bits in range(1, 7):
        chosen = lower_blocks(bits)
        right = [dot_ff(jnp.where(chosen, a, 0.0), t) for a, t in zip(systems, found)]
        found = [t - dot_ff(t, r) for t, r in zip(found, right)]
    return found


def run_maps(keys, values, beta_logits, decay_logits, extra_rows, speed):
    row, col = iota((RUN, RUN), 0), iota((RUN, RUN), 1)
    causal = row >= col
    systems, trails, betas, grown, lasts = [], [], [], [], []
    for p in range(2):
        beta_col = sigmoid(beta_logits[p])
        pace_col = softplus(decay_logits[p])
        pace_row = jnp.sum(jnp.where(row == col, pace_col, 0.0), axis=0, keepdims=True)
        fade_row = extra_rows[p] - speed * pace_row
        cum_col = jnp.sum(jnp.where(causal, fade_row, 0.0), axis=1, keepdims=True)
        cum_row = jnp.sum(jnp.where(row == col, cum_col, 0.0), axis=0, keepdims=True)
        beta_row = jnp.sum(jnp.where(row == col, beta_col, 0.0), axis=0, keepdims=True)
        last = cum_row[:, RUN - 1 :]
        within = jnp.where(causal, jnp.exp(jnp.where(causal, cum_col - cum_row, 0.0)), 0.0)
        gram = dot_nt(keys[p], keys[p])
        systems.append(jnp.where(row > col, gram * within * beta_col, 0.0))
        trails.append(keys[p].astype(f32).T * jnp.exp(last - cum_row))
        betas.append(beta_row)
        grown.append(jnp.exp(cum_row))
        lasts.append(jnp.exp(last))
    solved = inverses([systems[0][:128, :128], systems[0][128:, 128:],
                       systems[1][:128, :128], systems[1][128:, 128:]])
    maps = []
    diagonal = iota((128, 128), 0) == iota((128, 128), 1)
    for p in range(2):
        second = dot_ff(trails[p][:, 128:], solved[2 * p + 1])
        first = trails[p][:, :128] - dot_ff(second, systems[p][128:, :128])
        first = dot_ff(first, solved[2 * p])
        writes = jnp.concatenate([first, second], axis=1) * betas[p]
        offset = dot_fb(writes, values[p])
        moves = jnp.where(diagonal, lasts[p], 0.0) - dot_fb(writes * grown[p], keys[p])
        maps.append(jnp.concatenate([moves, offset], axis=1))
    return maps


def kernel(
    x_hbm, fg_hbm, wk_hbm, wv_hbm, wq_hbm, wz_hbm, wb_hbm, wd_hbm, speed_hbm, extra_hbm, gain_hbm, wo_hbm,
    cache_ref, step_ref,
    chunks, wkv, wqz, wlogit, wl, wo, fg, extra, gain, speeds,
    acc, acc_l, facc, own_map, other_map, blocks, state_out, state_in, parts_out, parts_in, row_out, row_in,
    load_sem, gather_send, ax_sem, ay_sem, by_sem, bx_sem,
    swap_send, swap_recv, ring_send, up_sem, down_sem, part_send, part_recv,
):
    z, c = lax.axis_index("z"), lax.axis_index("c")
    y, x = lax.axis_index("y"), lax.axis_index("x")
    mine = y * NX + x

    def ring(at, step, size):
        return lax.rem(at + (step % size), size)

    def slot(yy, xx):
        return yy * NX + xx

    def load(src, dst, sem):
        copy = pltpu.make_async_copy(src, dst, load_sem.at[sem])
        copy.start()
        return copy

    own_load = load(x_hbm, chunks.at[mine], 0)
    logit_loads = [
        load(wb_hbm, wlogit.at[pl.ds(0, 32)], 1),
        load(wd_hbm, wlogit.at[pl.ds(32, 32)], 2),
    ]
    early_loads = [
        load(fg_hbm, fg, 3),
        load(wk_hbm, wkv.at[:, pl.ds(0, 128)], 4),
        load(wv_hbm, wkv.at[:, pl.ds(128, 128)], 5),
        load(wq_hbm, wqz.at[:, pl.ds(0, 128)], 6),
        load(wz_hbm, wqz.at[:, pl.ds(128, 128)], 7),
    ]
    late_loads = [
        load(extra_hbm, extra, 8), load(gain_hbm, gain, 9), load(wo_hbm, wo, 10), load(speed_hbm, speeds, 11)
    ]

    barrier = pltpu.get_barrier_semaphore()
    for axis, at, size in (("x", x, NX), ("y", y, NY), ("z", z, NZ)):
        for step in (1, -1):
            pl.semaphore_signal(barrier, inc=1, device_id={axis: ring(at, step, size)}, device_id_type=MESH)
    pl.semaphore_signal(barrier, inc=1, device_id={"c": 1 - c}, device_id_type=MESH)
    own_load.wait()
    pl.semaphore_wait(barrier, 7)

    y_to = ({"y": ring(y, 1, NY)}, {"y": ring(y, -1, NY)})
    x_to = ({"x": ring(x, 1, NX)}, {"x": ring(x, -1, NX)})
    sign = (-1, 1)

    def chunk_copy(yy, xx, rows, sem, to):
        view = chunks.at[slot(yy, xx), pl.ds(rows[0], rows[1])]
        return pltpu.make_async_remote_copy(
            src_ref=view, dst_ref=view, send_sem=gather_send, recv_sem=sem, device_id=to, device_id_type=MESH
        )

    def ax(k, h, start):
        xx = ring(x, sign[k] * (h - 1 if start else h), NX)
        copy = chunk_copy(y, xx, A if h < 2 else A_HALF[k], ax_sem.at[k, h - 1], x_to[k])
        copy.start() if start else copy.wait_recv()

    def ay(k, h, j, start):
        yy = ring(y, sign[k] * (h - 1 if start else h), NY)
        copy = chunk_copy(yy, ring(x, j, NX), A if h < 4 else A_HALF[k], ay_sem.at[k, h - 1, j], y_to[k])
        copy.start() if start else copy.wait_recv()

    def by(k, h, start):
        yy = ring(y, sign[k] * (h - 1 if start else h), NY)
        copy = chunk_copy(yy, x, B if h < 4 else B_HALF[k], by_sem.at[k, h - 1], y_to[k])
        copy.start() if start else copy.wait_recv()

    def bx(k, h, j, start):
        xx = ring(x, sign[k] * (h - 1 if start else h), NX)
        copy = chunk_copy(ring(y, j, NY), xx, B if h < 2 else B_HALF[k], bx_sem.at[k, h - 1, j % NY], x_to[k])
        copy.start() if start else copy.wait_recv()

    both = (0, 1)

    def project(steps):
        def one(yy):
            row = pl.multiple_of(yy * KEEP, KEEP)
            left = jnp.concatenate([chunks[yy * NX + i] for i in range(NX)], axis=1)
            acc[...] += dot(left, wkv[pl.ds(row, KEEP), :])
            acc_l[...] += dot_nt(left, wl[:, pl.ds(row, KEEP)])

        for step in steps:
            one(ring(y, step, NY))

    def bx_first(j):
        for k in both:
            bx(k, 1, j, False)
            bx(k, 2, j, True)

    def bx_last(j):
        for k in both:
            bx(k, 2, j, False)

    def ay_pass(h, j):
        for k in both:
            ay(k, h, j, False)
            if h < 4:
                ay(k, h + 1, j, True)

    def by_pass(h):
        for k in both:
            by(k, h, False)
            if h < 4:
                by(k, h + 1, True)
        for j in (-h, h) if h < 4 else (4,):
            for k in both:
                bx(k, 1, j, True)

    for k in both:
        by(k, 1, True)
        ax(k, 1, True)
    for k in both:
        bx(k, 1, 0, True)
        ay(k, 1, 0, True)

    for copy in logit_loads:
        copy.wait()
    pick_row, pick_col = iota((16, 64), 0), iota((16, 64), 1)
    pick = ((pick_row == 0) & (pick_col == mine)) | ((pick_row == 1) & (pick_col == mine + 32))
    wl[...] = dot(jnp.where(pick, 1.0, 0.0).astype(bf16), wlogit[...]).astype(bf16)
    facc[...] = jnp.zeros_like(facc)
    acc[...] = jnp.zeros_like(acc)
    acc_l[...] = jnp.zeros_like(acc_l)

    def first_step(i, carry):
        at = pl.multiple_of(i * KEEP, KEEP)
        left = fg[:, pl.ds(at, KEEP)]
        facc[:, 0:256] += dot(left, wkv[pl.ds(at, KEEP), :])
        facc[:, 256:512] += dot(left, wqz[pl.ds(at, KEEP), :])
        facc[:, 512:528] += dot_nt(left, wl[:, pl.ds(at, KEEP)])
        return carry

    for k in both:
        ax(k, 1, False)
        ax(k, 2, True)
    for k in both:
        by(k, 1, False)
        by(k, 2, True)
    for j in (1, 3):
        for k in both:
            ay(k, 1, j, True)
    for j in (-1, 1):
        for k in both:
            bx(k, 1, j, True)
    bx_first(0)
    ay_pass(1, 0)
    for k in both:
        ax(k, 2, False)
    for k in both:
        ay(k, 1, 2, True)
    for copy in early_loads:
        copy.wait()

    @pl.when(c == 1)
    def _():
        lax.fori_loop(0, WIDTH // KEEP, first_step, 0)

    by_pass(2)
    bx_first(-1)
    ay_pass(1, 1)
    ay_pass(1, 3)
    bx_first(1)
    bx_last(0)
    ay_pass(1, 2)
    by_pass(3)
    ay_pass(2, 0)
    project([0])
    ay_pass(2, 1)
    bx_first(-2)
    ay_pass(2, 3)
    bx_first(2)
    bx_last(-1)
    bx_last(1)
    ay_pass(2, 2)
    by_pass(4)
    ay_pass(3, 0)
    bx_first(-3)
    project([-1])
    ay_pass(3, 1)
    bx_first(3)
    ay_pass(3, 3)
    project([1])
    bx_last(-2)
    bx_last(2)
    ay_pass(3, 2)
    bx_first(4)
    project([-2, 2])
    bx_last(-3)
    bx_last(3)
    project([-3, 3])
    for j in range(NX):
        ay_pass(4, j)
    bx_last(4)
    project([4])

    for copy in late_loads:
        copy.wait()
    speed = jnp.sum(jnp.where(iota((1, NT), 1) == mine, speeds[...], 0.0), axis=1, keepdims=True)
    keys = unit(silu(acc[:, 0:128])).astype(bf16)
    values = silu(acc[:, 128:256]).astype(bf16)
    logits = acc_l[...].astype(bf16).astype(f32)
    maps = run_maps(
        [keys[:RUN], keys[RUN:]],
        [values[:RUN], values[RUN:]],
        [logits[:RUN, 0:1], logits[RUN:, 0:1]],
        [logits[:RUN, 1:2], logits[RUN:, 1:2]],
        [extra[0], extra[1]],
        speed,
    )

    other_core = {"c": 1 - c}

    def swap(src, dst, i):
        return pltpu.make_async_remote_copy(
            src_ref=src, dst_ref=dst, send_sem=swap_send.at[i], recv_sem=swap_recv.at[i],
            device_id=other_core, device_id_type=MESH,
        )

    both_prompts = (0, 1)
    map_swap = swap(own_map, other_map, 0)
    state_swap = swap(state_out, state_in, 1)
    row_swap = swap(row_out, row_in, 2)

    @pl.when(c == 0)
    def _():
        own_map[0] = maps[0].astype(bf16)
        own_map[1] = maps[1].astype(bf16)
        map_swap.start()
        state_swap.wait_recv()
        cache_ref[...] = state_in[...]
        row_swap.wait_recv()
        step_ref[...] = row_in[...].astype(bf16)
        map_swap.wait_send()

    @pl.when(c == 1)
    def _():
        first = facc[...]
        new_key = unit(silu(first[:, 0:128]))
        new_value = silu(first[:, 128:256])
        new_query = unit(silu(first[:, 256:384]))
        out_gate = silu(first[:, 384:512])
        new_beta = sigmoid(first[:, 512:513])
        new_decay = jnp.exp(-speed * softplus(first[:, 513:514]))
        meeting = jnp.sum(new_key * new_query, axis=-1, keepdims=True)
        carried_query = new_decay * (new_query - new_beta * new_key * meeting)
        own_write = new_beta * new_value * meeting

        zeros = jnp.zeros((128, 128), f32)
        eye = (iota((128, 128), 0) == iota((128, 128), 1)).astype(f32)

        def with_offset(product, offset):
            return jnp.concatenate([product[:, :128], product[:, 128:] + offset], axis=1)

        z_to = ({"z": ring(z, 1, NZ)}, {"z": ring(z, -1, NZ)})
        z_sem = (up_sem, down_sem)
        per_prompt = PIECES // 2
        piece_rows = 128 // per_prompt

        def hop(k, h, q, start):
            zz = ring(z, sign[k] * (h - 1 if start else h), NZ)
            view = blocks.at[zz, q // per_prompt, pl.ds(q % per_prompt * piece_rows, piece_rows)]
            copy = pltpu.make_async_remote_copy(
                src_ref=view, dst_ref=view, send_sem=ring_send, recv_sem=z_sem[k].at[h - 1, q],
                device_id=z_to[k], device_id_type=MESH,
            )
            copy.start() if start else copy.wait_recv()

        map_swap.wait_recv()
        pair = []
        for p in both_prompts:
            early, late = other_map[p], maps[p]
            pair.append(with_offset(dot_fb(late[:, :128], early), late[:, 128:]))
            blocks[z, p] = pair[p].astype(bf16)
            for q in range(p * per_prompt, (p + 1) * per_prompt):
                for k in both:
                    hop(k, 1, q, True)

        limit = (UP, DOWN)
        before = [jnp.concatenate([eye, zeros], axis=1)] * 2
        after = [jnp.concatenate([eye, zeros], axis=1)] * 2
        start_state = [jnp.concatenate([zeros, zeros], axis=1)] * 2
        reader = [
            jnp.concatenate(
                [jnp.where(iota((8, 128), 0) == 0, carried_query[p : p + 1], 0.0), jnp.zeros((8, 128), f32)], axis=1
            )
            for p in both_prompts
        ]
        for h in range(1, UP + 1):
            for q in range(PIECES):
                for k in both:
                    if h <= limit[k]:
                        hop(k, h, q, False)
                        if h < limit[k]:
                            hop(k, h + 1, q, True)
            for p in both_prompts:
                block = blocks[ring(z, -h, NZ), p]
                stacked = jnp.concatenate([before[p], reader[p]], axis=0)
                grown = with_offset(dot_fb(stacked[:, :128], block), stacked[:, 128:])
                earlier = z >= h
                before[p] = jnp.where(earlier, grown[:128], before[p])
                reader[p] = jnp.where(earlier, reader[p], grown[128:])
                if h <= DOWN:
                    block = blocks[ring(z, h, NZ), p]
                    later = z + h < NZ
                    taken = jnp.where(later, after[p], start_state[p])
                    grown = dot_bf(block[:, :128], taken)
                    grown = with_offset(grown, block[:, 128:].astype(f32))
                    after[p] = jnp.where(later, grown, after[p])
                    start_state[p] = jnp.where(later, start_state[p], grown)

        enter, seconds, reads = [], [], []
        for p in both_prompts:
            enter.append(dot_ff(before[p][:, :128], start_state[p][:, 128:]) + before[p][:, 128:])
            seconds.append(dot_ff(pair[p][:, :128], enter[p]) + pair[p][:, 128:])
            tail = [dot_ff(reader[p][:, :128], after[p][:, i * 128 : (i + 1) * 128]) for i in range(2)]
            read = dot_ff(tail[0], seconds[p]) + tail[1] + reader[p][:, 128:]
            reads.append(read[0:1])
        read = jnp.concatenate(reads, axis=0) + own_write
        normed = read * lax.rsqrt(jnp.mean(read * read, axis=-1, keepdims=True) + norm_eps) * gain[...] * out_gate
        partial = dot(normed.astype(bf16), wo[...])
        for t in range(NT):
            parts_out[t] = partial[:, t * 128 : (t + 1) * 128]

        steps = [(dy, dx) for dy in range(NY) for dx in range(NX) if dy or dx]
        steps.sort(key=lambda s: -min(s[0], NY - s[0]) - min(s[1], NX - s[1]))
        for i, (dy, dx) in enumerate(steps):
            yy, xx = ring(y, dy, NY), ring(x, dx, NX)
            pltpu.make_async_remote_copy(
                src_ref=parts_out.at[slot(yy, xx)], dst_ref=parts_in.at[i], send_sem=part_send, recv_sem=part_recv,
                device_id={"y": yy, "x": xx}, device_id_type=MESH,
            ).start()
        for p in both_prompts:
            early = other_map[p]
            state_out[p] = (dot_bf(early[:, :128], enter[p]) + early[:, 128:].astype(f32)).astype(bf16)
        state_swap.start()
        for p in both_prompts:
            cache_ref[p] = seconds[p].astype(bf16)
        total = parts_out[mine]
        pltpu.make_async_copy(parts_in, parts_in, part_recv).wait()
        total = total + jnp.sum(parts_in[...], axis=0)
        row_out[...] = total
        row_swap.start()
        step_ref[...] = total.astype(bf16)
        state_swap.wait_send()
        row_swap.wait_send()
        sent = blocks.at[pl.ds(0, UP + DOWN)]
        pltpu.make_async_copy(sent, sent, ring_send).wait()
        pltpu.make_async_copy(parts_in, parts_in, part_send).wait()

    sent = chunks.at[pl.ds(0, NT - 1)]
    pltpu.make_async_copy(sent, sent, gather_send).wait()


def body(
    context_activations,
    first_generated_activation,
    address_projection,
    payload_projection,
    lookup_projection,
    exit_gating_projection,
    writing_intensity_projection,
    fading_projection,
    channel_fading_speed,
    extra_fading_log,
    readout_normalizer_gain,
    exit_projection,
):
    hbm = pl.BlockSpec(memory_space=pltpu.HBM)
    vmem = pl.BlockSpec(memory_space=pltpu.VMEM)
    dma = pltpu.SemaphoreType.DMA
    cache, step = pl.pallas_call(
        kernel,
        out_shape=(jax.ShapeDtypeStruct((2, HEAD, HEAD), bf16), jax.ShapeDtypeStruct((2, 128), bf16)),
        in_specs=[hbm] * 12,
        out_specs=(vmem, vmem),
        scratch_shapes=[
            pltpu.VMEM((NT, ROWS, 128), bf16),
            pltpu.VMEM((WIDTH, 256), bf16),
            pltpu.VMEM((WIDTH, 256), bf16),
            pltpu.VMEM((64, WIDTH), bf16),
            pltpu.VMEM((16, WIDTH), bf16),
            pltpu.VMEM((HEAD, WIDTH), bf16),
            pltpu.VMEM((2, WIDTH), bf16),
            pltpu.VMEM((2, 1, RUN), f32),
            pltpu.VMEM((1, HEAD), f32),
            pltpu.VMEM((1, NT), f32),
            pltpu.VMEM((ROWS, 256), f32),
            pltpu.VMEM((ROWS, 16), f32),
            pltpu.VMEM((2, 528), f32),
            pltpu.VMEM((2, 128, 256), bf16),
            pltpu.VMEM((2, 128, 256), bf16),
            pltpu.VMEM((NZ, 2, 128, 256), bf16),
            pltpu.VMEM((2, 128, 128), bf16),
            pltpu.VMEM((2, 128, 128), bf16),
            pltpu.VMEM((NT, 2, 128), f32),
            pltpu.VMEM((NT - 1, 2, 128), f32),
            pltpu.VMEM((2, 128), f32),
            pltpu.VMEM((2, 128), f32),
            dma((12,)),
            dma,
            dma((2, 2)),
            dma((2, 4, NX)),
            dma((2, 4)),
            dma((2, 2, NY)),
            dma((3,)),
            dma((3,)),
            dma,
            dma((UP, PIECES)),
            dma((DOWN, PIECES)),
            dma,
            dma,
        ],
        compiler_params=pltpu.CompilerParams(
            collective_id=0, has_side_effects=True, vmem_limit_bytes=67_043_328
        ),
    )(
        context_activations.reshape(ROWS, 128),
        first_generated_activation,
        address_projection,
        payload_projection,
        lookup_projection,
        exit_gating_projection,
        writing_intensity_projection.T,
        fading_projection.T,
        channel_fading_speed.reshape(1, NT),
        jnp.transpose(extra_fading_log, (0, 2, 1)),
        readout_normalizer_gain.reshape(1, HEAD),
        exit_projection,
    )
    return cache.reshape(2, 1, 1, HEAD, HEAD), step


def solution(mesh):
    torus = Mesh(mesh.devices.reshape(NZ, NC, NY, NX), ("z", "c", "y", "x"))
    SP, TP = ("z", "c"), ("y", "x")
    in_specs = (
        P(None, SP, TP),
        P(),
        P(None, TP),
        P(None, TP),
        P(None, TP),
        P(None, TP),
        P(),
        P(),
        P(),
        P(None, SP, TP),
        P(),
        P(TP, None),
    )
    out_specs = (P(None, SP, TP, None, None), P(None, TP))
    return jax.shard_map(body, mesh=torus, in_specs=in_specs, out_specs=out_specs, check_vma=False)
```
